32 devices in a mesh: sp: 8 (over z, x), dp: 4 (over y, core).
Axes of the slice: x: 2, y: 2, z: 4, core: 2. Of those that a mesh axis runs over, the one named last changes fastest.
Arguments:
- query_rows: bfloat16 [4, 1024, 2048], P('dp', 'sp'), may hold values from -6 to 6
- key_rows: bfloat16 [4, 1024, 2048], P('dp', 'sp'), may hold values from -6 to 6
- value_rows: bfloat16 [4, 1024, 2048], P('dp', 'sp'), may hold values from -6 to 6
- decay_low: bfloat16 [4, 1024, 128], P('dp', 'sp'), may hold values from -5 to 5
- rate_low: bfloat16 [4, 1024, 128], P('dp', 'sp'), may hold values from -4 to 4
- decay_up: bfloat16 [128, 2048], replicated, may hold values from -0.5 to 0.5
- rate_up: bfloat16 [128, 2048], replicated, may hold values from -0.5 to 0.5
- decay_base: float32 [2048], replicated, may hold values from -12 to -2
- norm_gain: float32 [2048], replicated, may hold values from 0.1 to 1.9
- out_weight: bfloat16 [2048, 2048], P(None, 'dp'), may hold values from -0.125 to 0.125
Outputs:
- layer_out: bfloat16 [4, 1024, 2048], P('dp', 'sp')
The draws below stay inside these ranges and needn't reach their ends.
All inputs are finite; a program needn't handle non-finite values.
Results may differ from the reference program's by a relative error of at most 0.005.
Values may be sent and summed in bfloat16 or wider, within the bound.
A program may use at most 128 MiB of HBM per device.

```python
import jax
import jax.numpy as jnp
from jax import lax

D = 2048
HEADS = 32
HEAD = 64
LOW = 128
TOK_DEV = 128
WIDTH = 2048
LENGTH = 1024
BATCH = 4


def draw_decay_low(key, part):
    noise = jnp.clip(jax.random.normal(jax.random.fold_in(key, 11), (BATCH, LENGTH, LOW), jnp.float32), -4.0, 4.0)
    offsets = jax.random.uniform(jax.random.fold_in(key, 12), (BATCH, LENGTH // TOK_DEV, 1), jnp.float32, minval=-1.0, maxval=1.0)
    total = noise + jnp.repeat(offsets, TOK_DEV, axis=1)
    return jnp.clip(total, -5.0, 5.0).astype(jnp.bfloat16)


def draw_decay_base(key, part):
    picks = jax.random.randint(jax.random.fold_in(key, 21), (HEADS, 1), 0, 16)
    quick = picks < 8
    slow_rate = jax.random.uniform(jax.random.fold_in(key, 22), (HEADS, HEAD), jnp.float32, minval=0.2, maxval=1.0) / LENGTH
    quick_rate = jax.random.uniform(jax.random.fold_in(key, 23), (HEADS, HEAD), jnp.float32, minval=0.01, maxval=0.033)
    chosen = jnp.where(quick, quick_rate, slow_rate)
    return jnp.clip(jnp.log(chosen) + 0.5, -12.0, -2.0).reshape(WIDTH).astype(jnp.float32)


def block_levels(key, extent, pieces, least, top_value):
    level = 1.0
    for dim, parts in pieces:
        heights = jax.random.uniform(jax.random.fold_in(jax.random.fold_in(key, 6), dim), (parts,), jnp.float32, least / len(pieces), top_value / len(pieces))
        level = level * jnp.repeat(jnp.exp(heights), extent[dim] // parts).reshape((-1,) + (1,) * (len(extent) - 1 - dim))
    return level


def gaussian(stream_key, dims, deviation, reach, cuts=(), held_as=jnp.bfloat16):
    values = deviation * jax.random.normal(stream_key, dims, jnp.float32)
    if cuts:
        values = values * block_levels(stream_key, dims, cuts, -0.22, 0.18)
    return jnp.clip(values, -reach, reach).astype(held_as)


def setup_inputs(seed: int = 0) -> dict:
    splits = jax.random.split(jax.random.key(seed), 11)
    query_rows = gaussian(splits[0], (BATCH, LENGTH, WIDTH), 1.0, 6.0, ((0, 4), (1, 8)))
    key_rows = gaussian(splits[1], (BATCH, LENGTH, WIDTH), 1.0, 6.0, ((0, 4), (1, 8)))
    value_rows = gaussian(splits[2], (BATCH, LENGTH, WIDTH), 1.0, 6.0, ((0, 4), (1, 8)))
    decay_low = draw_decay_low(jax.random.fold_in(splits[10], 71), 0)
    rate_low = gaussian(splits[4], (BATCH, LENGTH, LOW), 1.0, 4.0, ((0, 4), (1, 8)))
    decay_up = gaussian(splits[5], (LOW, WIDTH), LOW ** -0.5, 0.5)
    rate_up = gaussian(splits[6], (LOW, WIDTH), LOW ** -0.5, 0.5)
    decay_base = draw_decay_base(jax.random.fold_in(splits[10], 71), 0)
    norm_gain = jnp.clip(1.0 + 0.18 * jax.random.normal(splits[8], (WIDTH,), jnp.float32), 0.1, 1.9)
    out_weight = gaussian(splits[9], (WIDTH, D), WIDTH ** -0.5, 0.125, ((1, 4),))
    return {"query_rows": query_rows, "key_rows": key_rows, "value_rows": value_rows, "decay_low": decay_low, "rate_low": rate_low, "decay_up": decay_up, "rate_up": rate_up, "decay_base": decay_base, "norm_gain": norm_gain, "out_weight": out_weight}


HIGHEST = lax.Precision.HIGHEST

def reference(query_rows, key_rows, value_rows, decay_low, rate_low, decay_up, rate_up, decay_base, norm_gain, out_weight):
    heads = query_rows.shape[2] // HEAD

    def one_sequence(inputs):
        reads, keyed, valued, low_decay, low_rate = inputs
        positions = reads.shape[0]
        squashed = jnp.tanh(low_decay.astype(jnp.float32)).astype(jnp.bfloat16)
        decay_pre = (decay_base + jnp.dot(squashed, decay_up, preferred_element_type=jnp.float32)).astype(jnp.bfloat16)
        rate_pre = jnp.dot(low_rate, rate_up, preferred_element_type=jnp.float32).astype(jnp.bfloat16)
        log_decay = -jnp.exp(-jax.nn.softplus(-decay_pre.astype(jnp.float32)) - 0.5)
        rate = jax.nn.sigmoid(rate_pre.astype(jnp.float32))
        head_shape = (positions, heads, HEAD)
        query_heads = reads.astype(jnp.float32).reshape(head_shape)
        key_heads = keyed.astype(jnp.float32).reshape(head_shape)
        value_heads = valued.astype(jnp.float32).reshape(head_shape)
        decay_heads = jnp.exp(log_decay).reshape(head_shape)
        unit_keys = key_heads * lax.rsqrt(1.0 + lax.optimization_barrier(jnp.sum(key_heads * key_heads, axis=-1, keepdims=True)))
        erase = unit_keys * rate.reshape(head_shape)

        def advance(state, inputs_now):
            query_now, decay_now, key_now, value_now, unit_now, erase_now = inputs_now
            removed = jnp.einsum('hvk,hk->hv', state, unit_now, precision=HIGHEST)
            state = state * decay_now[:, None, :] - removed[:, :, None] * erase_now[:, None, :] + value_now[:, :, None] * key_now[:, None, :]
            return (state, jnp.einsum('hvk,hk->hv', state, query_now, precision=HIGHEST))
        initial = jnp.zeros((heads, HEAD, HEAD), jnp.float32)
        _, readout = lax.scan(advance, initial, (query_heads, decay_heads, key_heads, value_heads, unit_keys, erase))
        average = lax.optimization_barrier(jnp.mean(readout, axis=-1, keepdims=True))
        centred = readout - average
        variance = lax.optimization_barrier(jnp.mean(centred * centred, axis=-1, keepdims=True))
        normed = (centred * lax.rsqrt(variance + 1.0)).reshape(positions, heads * HEAD)
        mix = (normed * norm_gain).astype(jnp.bfloat16)
        return jnp.dot(mix, out_weight, preferred_element_type=jnp.float32).astype(jnp.bfloat16)
    return lax.map(one_sequence, (query_rows, key_rows, value_rows, decay_low, rate_low))
```

```python
import functools
import math

import jax
import jax.numpy as jnp
from jax import lax
from jax.experimental import pallas as pl
from jax.experimental.pallas import tpu as pltpu
from jax.sharding import PartitionSpec as P

HEAD = 64
PAIR = 2 * HEAD

F32 = jnp.float32
BF16 = jnp.bfloat16


def mm(left, right):
    return lax.dot_general(left, right, (((1,), (0,)), ((), ())), preferred_element_type=F32)


def mm_nt(left, right):
    return lax.dot_general(left, right, (((1,), (1,)), ((), ())), preferred_element_type=F32)


def mm_tn(left, right):
    return lax.dot_general(left, right, (((0,), (0,)), ((), ())), preferred_element_type=F32)


def split(x):
    high = x.astype(BF16)
    return high, (x - high.astype(F32)).astype(BF16)


def mm3(left, right, form=mm):
    return form(left[0], right[0]) + form(left[0], right[1]) + form(left[1], right[0])


def iota(shape, dim):
    return lax.broadcasted_iota(jnp.int32, shape, dim)


def first_half(shape):
    return iota(shape, len(shape) - 1) < HEAD


def stack_pair(x):
    here = lax.rem(iota(x.shape, 1), PAIR) < HEAD
    zero = jnp.zeros_like(x)
    return jnp.concatenate([jnp.where(here, x, zero), jnp.where(here, zero, x)], axis=0)


def head_ones(scale):
    row = iota((2 * PAIR, PAIR), 0)
    col = iota((2 * PAIR, PAIR), 1)
    same = (lax.rem(row, PAIR) // HEAD) == (col // HEAD)
    return jnp.where(same, F32(scale), F32(0.0)).astype(BF16)


def head_sum(x, ones):
    return mm(jnp.concatenate(split(x), axis=1), ones)


def inverse_levels(strict_parts, size):
    row = iota((size, size), 0)
    col = iota((size, size), 1)
    eye = jnp.where(row == col, F32(1.0), F32(0.0))
    found = None
    block = 1
    while block < size:
        pick = (row // (2 * block) == col // (2 * block)) & (row // block != col // block) & (row > col)
        pieces = [jnp.where(pick, high, jnp.zeros_like(high)) for high, _ in strict_parts]
        if found is None:
            found = [eye.astype(BF16) - p for p in pieces]
        else:
            right = [mm(p, x).astype(BF16) for p, x in zip(pieces, found)]
            found = [x - mm(x, y).astype(BF16) for x, y in zip(found, right)]
        block *= 2
    out = []
    for (high, low), x in zip(strict_parts, found):
        product = mm(jnp.concatenate([high, low], axis=1), jnp.concatenate([x, x], axis=0))
        residual = ((eye - x.astype(F32)) - product).astype(BF16)
        out.append((x, mm(x, residual).astype(BF16)))
    return out


def gates(squashed, rate_low, decay_up, rate_up, base):
    decay_pre = (base + mm(squashed, decay_up)).astype(BF16).astype(F32)
    rate_pre = mm(rate_low, rate_up).astype(BF16).astype(F32)
    log_decay = -math.exp(-0.5) / (1.0 + jnp.exp(-decay_pre))
    rate = 1.0 / (1.0 + jnp.exp(-rate_pre))
    return log_decay, rate


def local_pairs(pairs):
    size = pairs[0][0].shape[0]
    middle = size // 2
    row = iota((size, size), 0)
    col = iota((size, size), 1)
    strict = row > col
    within = row >= col
    upto = jnp.where(within, F32(1.0), F32(0.0)).astype(BF16)
    upto = jnp.concatenate([upto, upto], axis=1)
    ones = head_ones(1.0)
    made = []
    strict_parts = []
    for q, k, v, log_decay, rate in pairs:
        q = q.astype(F32)
        k = k.astype(F32)
        running = mm(upto, jnp.concatenate(split(log_decay), axis=0))
        centre = running[middle : middle + 1]
        final = running[size - 1 :]
        ahead = jnp.exp(running - centre)
        ahead_before = jnp.exp(running - log_decay - centre)
        behind = jnp.exp(centre - running)
        unit = k * lax.rsqrt(1.0 + head_sum(k * k, ones))
        erase = unit * rate
        at_centre = jnp.exp(centre)
        at_end = jnp.exp(final - centre)
        read_mid = q * ahead
        erase_from = unit * ahead_before
        key_to = k * behind
        erase_to = erase * behind
        left = split(jnp.concatenate([stack_pair(erase_from), stack_pair(read_mid)], axis=0))
        right = split(jnp.concatenate([key_to, erase_to], axis=0))
        grid = mm_nt(
            jnp.concatenate(left, axis=1), jnp.concatenate([right[0], right[0]], axis=1)
        ) + mm_nt(left[0], right[1])
        part = lambda i, j, keep: jnp.where(
            keep, grid[i * size : (i + 1) * size, j * size : (j + 1) * size], 0.0
        )
        key_pairs = split(jnp.concatenate([part(0, 0, strict), part(1, 0, strict)], axis=1))
        strict_parts += [split(part(0, 1, strict)), split(part(1, 1, strict))]
        read_keys = split(jnp.concatenate([part(2, 0, within), part(3, 0, within)], axis=1))
        read_erase = split(jnp.concatenate([part(2, 1, within), part(3, 1, within)], axis=1))
        values = stack_pair(v)
        carried = mm(key_pairs[0], values) + mm(key_pairs[1], values)
        kept = mm(read_keys[0], values) + mm(read_keys[1], values)
        sides = jnp.concatenate([erase_from * at_centre, carried], axis=1)
        made.append((
            v, sides, kept, read_erase, read_mid * at_centre,
            key_to * at_end, erase_to * at_end, jnp.exp(final),
        ))
    inverses = inverse_levels(strict_parts, size)
    out = []
    for i, (v, sides, kept, read_erase, read_start, key_end, erase_end, decay_all) in enumerate(made):
        xa, xb = inverses[2 * i], inverses[2 * i + 1]
        inv = tuple(jnp.concatenate([a, b], axis=1) for a, b in zip(xa, xb))
        solved = mm3(inv, split(stack_pair(sides)))
        parts = split(solved)
        taken = mm3(read_erase, tuple(stack_pair(p) for p in parts))
        read_state = read_start - taken[:, :PAIR]
        readout = kept - taken[:, PAIR:]
        key_parts = split(key_end)
        erase_parts = split(erase_end)
        moved = mm3(erase_parts, parts, mm_tn)
        gained = mm_tn(key_parts[0], v) + mm_tn(key_parts[1], v)
        row2 = iota((PAIR, PAIR), 0)
        col2 = iota((PAIR, PAIR), 1)
        transfer = jnp.where(row2 == col2, jnp.broadcast_to(decay_all, (PAIR, PAIR)), 0.0) - moved[:, :PAIR]
        added = gained - moved[:, PAIR:]
        half = first_half((HEAD, PAIR))
        fold = lambda x: jnp.where(half, x[:HEAD], x[HEAD:])
        out.append((fold(transfer), fold(added), read_state, readout))
    return out


def local_kernel(count, q_ref, k_ref, v_ref, low_ref, rate_ref, dup_ref, rup_ref, base_ref,
                 transfer_ref, added_ref, state_ref, readout_ref):
    squashed = jnp.tanh(low_ref[...].astype(F32)).astype(BF16)
    log_decay, rate = gates(squashed, rate_ref[...], dup_ref[...], rup_ref[...], base_ref[...])
    pairs = []
    for i in range(count):
        at = slice(i * PAIR, (i + 1) * PAIR)
        pairs.append((q_ref[:, at], k_ref[:, at], v_ref[:, at], log_decay[:, at], rate[:, at]))
    for i, (transfer, added, state, readout) in enumerate(local_pairs(pairs)):
        at = slice(i * PAIR, (i + 1) * PAIR)
        transfer_ref[:, at] = transfer
        added_ref[:, at] = added
        state_ref[:, at] = state
        readout_ref[:, at] = readout


def local_block(q, k, v, decay_low, rate_low, decay_up, rate_up, base):
    size, width = q.shape
    low = decay_low.shape[1]
    count = math.gcd(width // PAIR, 2)
    lanes = count * PAIR
    cols = lambda rows: pl.BlockSpec((rows, lanes), lambda i: (0, i))
    whole = pl.BlockSpec((size, low), lambda i: (0, 0))
    return pl.pallas_call(
        functools.partial(local_kernel, count),
        grid=(width // lanes,),
        in_specs=[cols(size)] * 3 + [whole] * 2 + [cols(low)] * 2 + [cols(1)],
        out_specs=[cols(HEAD), cols(HEAD), cols(size), cols(size)],
        out_shape=[
            jax.ShapeDtypeStruct((HEAD, width), F32),
            jax.ShapeDtypeStruct((HEAD, width), F32),
            jax.ShapeDtypeStruct((size, width), F32),
            jax.ShapeDtypeStruct((size, width), F32),
        ],
        cost_estimate=pl.CostEstimate(flops=10**10, bytes_accessed=10**7, transcendentals=0),
        name="local_block",
    )(q, k, v, decay_low, rate_low, decay_up, rate_up, base)


def chain_kernel(devices, group, transfer_ref, added_ref, state_ref, readout_ref, gain_ref,
                 mix_ref, start_buf, end_buf, send_sem, recv_sem):
    me = lax.axis_index("sp")
    groups = transfer_ref.shape[1] // group
    has_left = me > 0
    has_right = me < devices - 1
    barrier = pltpu.get_barrier_semaphore()

    @pl.when(has_left)
    def _():
        pl.semaphore_signal(barrier, inc=1, device_id={"sp": me - 1}, device_id_type=pl.DeviceIdType.MESH)

    @pl.when(has_right)
    def _():
        pl.semaphore_signal(barrier, inc=1, device_id={"sp": me + 1}, device_id_type=pl.DeviceIdType.MESH)

    pl.semaphore_wait(barrier, jnp.minimum(me, 1) + jnp.minimum(devices - 1 - me, 1))

    def copy(g):
        return pltpu.make_async_remote_copy(
            src_ref=end_buf.at[g],
            dst_ref=start_buf.at[g],
            send_sem=send_sem.at[g],
            recv_sem=recv_sem.at[g],
            device_id={"sp": lax.rem(me + 1, devices)},
            device_id_type=pl.DeviceIdType.MESH,
        )

    mean_ones = head_ones(1.0 / HEAD)

    @pl.when(jnp.logical_not(has_left))
    def _():
        start_buf[...] = jnp.zeros_like(start_buf)

    for g in range(groups):
        @pl.when(has_left)
        def _():
            copy(g).wait_recv()

        starts = []
        for i in range(group // PAIR):
            at = slice(g * group + i * PAIR, g * group + (i + 1) * PAIR)
            here = slice(i * PAIR, (i + 1) * PAIR)
            start = split(stack_pair(start_buf[g, :, here]))
            end_buf[g, :, here] = mm3(split(transfer_ref[:, at]), start) + added_ref[:, at]
            starts.append(start)

        @pl.when(has_right)
        def _():
            copy(g).start()

        for i, start in enumerate(starts):
            at = slice(g * group + i * PAIR, g * group + (i + 1) * PAIR)
            readout = mm3(split(state_ref[:, at]), start) + readout_ref[:, at]
            centred = readout - head_sum(readout, mean_ones)
            variance = head_sum(centred * centred, mean_ones)
            mix_ref[:, at] = (centred * lax.rsqrt(variance + 1.0) * gain_ref[:, at]).astype(BF16)

    @pl.when(has_right)
    def _():
        for g in range(groups):
            copy(g).wait_send()


def chain(devices, transfer, added, state, readout, gain):
    size, width = state.shape
    group = PAIR * math.gcd(width // PAIR, 2)
    groups = width // group
    vmem = pl.BlockSpec(memory_space=pltpu.VMEM)
    return pl.pallas_call(
        functools.partial(chain_kernel, devices, group),
        in_specs=[vmem] * 5,
        out_specs=vmem,
        out_shape=jax.ShapeDtypeStruct((size, width), BF16),
        scratch_shapes=[
            pltpu.VMEM((groups, HEAD, group), F32),
            pltpu.VMEM((groups, HEAD, group), F32),
            pltpu.SemaphoreType.DMA((groups,)),
            pltpu.SemaphoreType.DMA((groups,)),
        ],
        compiler_params=pltpu.CompilerParams(collective_id=0, has_side_effects=True),
        cost_estimate=pl.CostEstimate(flops=10**10, bytes_accessed=10**7, transcendentals=0),
        name="state_chain",
    )(transfer, added, state, readout, gain)


def per_device(devices, query_rows, key_rows, value_rows, decay_low, rate_low, decay_up, rate_up,
               decay_base, norm_gain, out_weight):
    weight = lax.all_gather(out_weight, "dp", axis=1, tiled=True)
    made = local_block(
        query_rows[0], key_rows[0], value_rows[0], decay_low[0], rate_low[0],
        decay_up, rate_up, decay_base[None],
    )
    mix = chain(devices, *made, norm_gain[None])
    return jnp.dot(mix, weight, preferred_element_type=F32).astype(BF16)[None]


def solution(mesh):
    in_specs = (
        P("dp", "sp", None),
        P("dp", "sp", None),
        P("dp", "sp", None),
        P("dp", "sp", None),
        P("dp", "sp", None),
        P(),
        P(),
        P(),
        P(),
        P(None, "dp"),
    )
    return jax.shard_map(
        functools.partial(per_device, mesh.shape["sp"]),
        mesh=mesh, in_specs=in_specs, out_specs=P("dp", "sp", None), check_vma=False,
    )
```

```python
import functools
import math

import jax
import jax.numpy as jnp
from jax import lax
from jax.experimental import pallas as pl
from jax.experimental.pallas import tpu as pltpu
from jax.sharding import PartitionSpec as P

HEAD = 64
PAIR = 2 * HEAD

F32 = jnp.float32
BF16 = jnp.bfloat16


def mm(left, right):
    return lax.dot_general(left, right, (((1,), (0,)), ((), ())), preferred_element_type=F32)


def mm_nt(left, right):
    return lax.dot_general(left, right, (((1,), (1,)), ((), ())), preferred_element_type=F32)


def mm_tn(left, right):
    return lax.dot_general(left, right, (((0,), (0,)), ((), ())), preferred_element_type=F32)


def split(x):
    high = x.astype(BF16)
    return high, (x - high.astype(F32)).astype(BF16)


def mm3(left, right, form=mm):
    return form(left[0], right[0]) + form(left[0], right[1]) + form(left[1], right[0])


def iota(shape, dim):
    return lax.broadcasted_iota(jnp.int32, shape, dim)


def first_half(shape):
    return iota(shape, len(shape) - 1) < HEAD


def stack_pair(x):
    here = lax.rem(iota(x.shape, 1), PAIR) < HEAD
    zero = jnp.zeros_like(x)
    return jnp.concatenate([jnp.where(here, x, zero), jnp.where(here, zero, x)], axis=0)


def head_ones(scale):
    row = iota((2 * PAIR, PAIR), 0)
    col = iota((2 * PAIR, PAIR), 1)
    same = (lax.rem(row, PAIR) // HEAD) == (col // HEAD)
    return jnp.where(same, F32(scale), F32(0.0)).astype(BF16)


def head_sum(x, ones):
    return mm(jnp.concatenate(split(x), axis=1), ones)


def inverse_levels(strict_parts, size):
    row = iota((size, size), 0)
    col = iota((size, size), 1)
    eye = jnp.where(row == col, F32(1.0), F32(0.0))
    found = None
    block = 1
    while block < size:
        pick = (row // (2 * block) == col // (2 * block)) & (row // block != col // block) & (row > col)
        pieces = [jnp.where(pick, high, jnp.zeros_like(high)) for high, _ in strict_parts]
        if found is None:
            found = [eye.astype(BF16) - p for p in pieces]
        else:
            right = [mm(p, x).astype(BF16) for p, x in zip(pieces, found)]
            found = [x - mm(x, y).astype(BF16) for x, y in zip(found, right)]
        block *= 2
    out = []
    for (high, low), x in zip(strict_parts, found):
        product = mm(jnp.concatenate([high, low], axis=1), jnp.concatenate([x, x], axis=0))
        residual = ((eye - x.astype(F32)) - product).astype(BF16)
        out.append((x, mm(x, residual).astype(BF16)))
    return out


def gates(squashed, rate_low, decay_up, rate_up, base):
    decay_pre = (base + mm(squashed, decay_up)).astype(BF16).astype(F32)
    rate_pre = mm(rate_low, rate_up).astype(BF16).astype(F32)
    log_decay = -math.exp(-0.5) / (1.0 + jnp.exp(-decay_pre))
    rate = 1.0 / (1.0 + jnp.exp(-rate_pre))
    return log_decay, rate


def local_pairs(pairs):
    size = pairs[0][0].shape[0]
    middle = size // 2
    row = iota((size, size), 0)
    col = iota((size, size), 1)
    strict = row > col
    within = row >= col
    upto = jnp.where(within, F32(1.0), F32(0.0)).astype(BF16)
    upto = jnp.concatenate([upto, upto], axis=1)
    ones = head_ones(1.0)
    made = []
    strict_parts = []
    for q, k, v, log_decay, rate in pairs:
        q = q.astype(F32)
        k = k.astype(F32)
        running = mm(upto, jnp.concatenate(split(log_decay), axis=0))
        centre = running[middle : middle + 1]
        final = running[size - 1 :]
        ahead = jnp.exp(running - centre)
        ahead_before = jnp.exp(running - log_decay - centre)
        behind = jnp.exp(centre - running)
        unit = k * lax.rsqrt(1.0 + head_sum(k * k, ones))
        erase = unit * rate
        at_centre = jnp.exp(centre)
        at_end = jnp.exp(final - centre)
        read_mid = q * ahead
        erase_from = unit * ahead_before
        key_to = k * behind
        erase_to = erase * behind
        left = split(jnp.concatenate([stack_pair(erase_from), stack_pair(read_mid)], axis=0))
        right = split(jnp.concatenate([key_to, erase_to], axis=0))
        grid = mm_nt(
            jnp.concatenate(left, axis=1), jnp.concatenate([right[0], right[0]], axis=1)
        ) + mm_nt(left[0], right[1])
        part = lambda i, j, keep: jnp.where(
            keep, grid[i * size : (i + 1) * size, j * size : (j + 1) * size], 0.0
        )
        key_pairs = split(jnp.concatenate([part(0, 0, strict), part(1, 0, strict)], axis=1))
        strict_parts += [split(part(0, 1, strict)), split(part(1, 1, strict))]
        read_keys = split(jnp.concatenate([part(2, 0, within), part(3, 0, within)], axis=1))
        read_erase = split(jnp.concatenate([part(2, 1, within), part(3, 1, within)], axis=1))
        values = stack_pair(v)
        carried = mm(key_pairs[0], values) + mm(key_pairs[1], values)
        kept = mm(read_keys[0], values) + mm(read_keys[1], values)
        sides = jnp.concatenate([erase_from * at_centre, carried], axis=1)
        made.append((
            v, sides, kept, read_erase, read_mid * at_centre,
            key_to * at_end, erase_to * at_end, jnp.exp(final),
        ))
    inverses = inverse_levels(strict_parts, size)
    out = []
    for i, (v, sides, kept, read_erase, read_start, key_end, erase_end, decay_all) in enumerate(made):
        xa, xb = inverses[2 * i], inverses[2 * i + 1]
        inv = tuple(jnp.concatenate([a, b], axis=1) for a, b in zip(xa, xb))
        solved = mm3(inv, split(stack_pair(sides)))
        parts = split(solved)
        taken = mm3(read_erase, tuple(stack_pair(p) for p in parts))
        read_state = read_start - taken[:, :PAIR]
        readout = kept - taken[:, PAIR:]
        key_parts = split(key_end)
        erase_parts = split(erase_end)
        moved = mm3(erase_parts, parts, mm_tn)
        gained = mm_tn(key_parts[0], v) + mm_tn(key_parts[1], v)
        row2 = iota((PAIR, PAIR), 0)
        col2 = iota((PAIR, PAIR), 1)
        transfer = jnp.where(row2 == col2, jnp.broadcast_to(decay_all, (PAIR, PAIR)), 0.0) - moved[:, :PAIR]
        added = gained - moved[:, PAIR:]
        half = first_half((HEAD, PAIR))
        fold = lambda x: jnp.where(half, x[:HEAD], x[HEAD:])
        out.append((fold(transfer), fold(added), read_state, readout))
    return out


def fused_kernel(devices, columns, lanes, pieces, q_ref, k_ref, v_ref, low_ref, rate_ref, dup_ref,
                 rup_ref, base_ref, gain_ref, weight_ref, out_ref, weights, transfer_ref, added_ref,
                 state_ref, readout_ref, mix_ref, start_buf, end_buf, own_sem, near_sem, far_send,
                 far_recv, pass_send, pass_recv, send_sem, recv_sem):
    me = lax.axis_index("sp")
    mine = lax.axis_index("dp")
    partner = mine + 1 - 2 * lax.rem(mine, 2)
    width = q_ref.shape[1]
    groups = width // lanes
    count = lanes // PAIR
    others = columns // 2 - 1
    cols = weight_ref.shape[1]
    piece = weight_ref.shape[0] // pieces
    has_left = me > 0
    has_right = me < devices - 1
    barrier = pltpu.get_barrier_semaphore()

    def greet(where):
        pl.semaphore_signal(barrier, inc=1, device_id=where, device_id_type=pl.DeviceIdType.MESH)

    def ahead_of(j):
        return lax.rem(mine + 2 * (j + 1), columns)

    def behind_of(j):
        return lax.rem(mine + columns - 2 * (j + 1), columns)

    def remote(src, dst, send, recv, where):
        return pltpu.make_async_remote_copy(
            src_ref=src, dst_ref=dst, send_sem=send, recv_sem=recv,
            device_id=where, device_id_type=pl.DeviceIdType.MESH,
        )

    greet({"dp": partner})
    for j in range(others):
        greet({"dp": ahead_of(j)})

    @pl.when(has_left)
    def _():
        greet({"sp": me - 1})

    @pl.when(has_right)
    def _():
        greet({"sp": me + 1})

    own = pltpu.make_async_copy(weight_ref, weights.at[mine], own_sem)
    own.start()
    pl.semaphore_wait(
        barrier, 1 + others + jnp.minimum(me, 1) + jnp.minimum(devices - 1 - me, 1)
    )

    def rows(c):
        return pl.ds(c * piece, piece)

    def far(j, c):
        return remote(
            weight_ref.at[rows(c)], weights.at[mine, rows(c)],
            far_send.at[j, c], far_recv.at[j, c], {"dp": ahead_of(j)},
        )

    def passed(j, c):
        return remote(
            weights.at[behind_of(j), rows(c)], weights.at[behind_of(j), rows(c)],
            pass_send.at[j, c], pass_recv.at[j, c], {"dp": partner},
        )

    near = remote(weight_ref, weights.at[mine], near_sem.at[0], near_sem.at[1], {"dp": partner})
    for j in range(others):
        for c in range(pieces):
            far(j, c).start()
    near.start()

    def forward(c):
        for j in range(others):
            far(j, c).wait_recv()
            passed(j, c).start()

    def local_step(g, carry):
        at = pl.ds(pl.multiple_of(g * lanes, lanes), lanes)
        squashed = jnp.tanh(low_ref[...].astype(F32)).astype(BF16)
        log_decay, rate = gates(
            squashed, rate_ref[...], dup_ref[:, at], rup_ref[:, at], base_ref[:, at]
        )
        q, k, v = q_ref[:, at], k_ref[:, at], v_ref[:, at]
        cut = lambda x, i: x[:, i * PAIR : (i + 1) * PAIR]
        pairs = [tuple(cut(x, i) for x in (q, k, v, log_decay, rate)) for i in range(count)]
        parts = list(zip(*local_pairs(pairs)))
        for ref, part in zip((transfer_ref, added_ref, state_ref, readout_ref), parts):
            ref[:, at] = jnp.concatenate(part, axis=1)
        return carry

    lax.fori_loop(0, groups, local_step, 0)
    early = pieces // 2
    for c in range(early):
        forward(c)

    def copy(g):
        return remote(
            end_buf.at[g], start_buf.at[g], send_sem.at[g], recv_sem.at[g],
            {"sp": lax.rem(me + 1, devices)},
        )

    mean_ones = head_ones(1.0 / HEAD)

    @pl.when(jnp.logical_not(has_left))
    def _():
        start_buf[...] = jnp.zeros_like(start_buf)

    for g in range(groups):
        @pl.when(has_left)
        def _():
            copy(g).wait_recv()

        starts = []
        for i in range(count):
            at = slice(g * lanes + i * PAIR, g * lanes + (i + 1) * PAIR)
            here = slice(i * PAIR, (i + 1) * PAIR)
            start = split(stack_pair(start_buf[g, :, here]))
            end_buf[g, :, here] = mm3(split(transfer_ref[:, at]), start) + added_ref[:, at]
            starts.append(start)

        @pl.when(has_right)
        def _():
            copy(g).start()

        for i, start in enumerate(starts):
            at = slice(g * lanes + i * PAIR, g * lanes + (i + 1) * PAIR)
            readout = mm3(split(state_ref[:, at]), start) + readout_ref[:, at]
            centred = readout - head_sum(readout, mean_ones)
            variance = head_sum(centred * centred, mean_ones)
            mix_ref[:, at] = (centred * lax.rsqrt(variance + 1.0) * gain_ref[:, at]).astype(BF16)

    for c in range(early, pieces):
        forward(c)

    def project(d):
        at = pl.ds(pl.multiple_of(d * cols, cols), cols)
        out_ref[:, at] = mm(mix_ref[...], weights[d]).astype(BF16)

    own.wait()
    project(mine)
    near.wait_recv()
    project(partner)
    for j in range(others):
        project(behind_of(j))
    for j in range(others):
        for c in range(pieces):
            passed(j, c).wait_recv()
        project(lax.rem(partner + columns - 2 * (j + 1), columns))

    near.wait_send()
    for j in range(others):
        for c in range(pieces):
            far(j, c).wait_send()
            passed(j, c).wait_send()

    @pl.when(has_right)
    def _():
        for g in range(groups):
            copy(g).wait_send()


def per_device(devices, columns, query_rows, key_rows, value_rows, decay_low, rate_low, decay_up,
               rate_up, decay_base, norm_gain, out_weight):
    q = query_rows[0]
    size, width = q.shape
    depth, cols = out_weight.shape
    lanes = PAIR * math.gcd(width // PAIR, 2)
    groups = width // lanes
    pieces = 4
    others = columns // 2 - 1
    vmem = pl.BlockSpec(memory_space=pltpu.VMEM)
    dma = lambda *dims: pltpu.SemaphoreType.DMA(dims)
    out = pl.pallas_call(
        functools.partial(fused_kernel, devices, columns, lanes, pieces),
        in_specs=[vmem] * 9 + [pl.BlockSpec(memory_space=pl.ANY)],
        out_specs=vmem,
        out_shape=jax.ShapeDtypeStruct((size, columns * cols), BF16),
        scratch_shapes=[
            pltpu.VMEM((columns, depth, cols), BF16),
            pltpu.VMEM((HEAD, width), F32),
            pltpu.VMEM((HEAD, width), F32),
            pltpu.VMEM((size, width), F32),
            pltpu.VMEM((size, width), F32),
            pltpu.VMEM((size, width), BF16),
            pltpu.VMEM((groups, HEAD, lanes), F32),
            pltpu.VMEM((groups, HEAD, lanes), F32),
            pltpu.SemaphoreType.DMA,
            dma(2),
            dma(others, pieces),
            dma(others, pieces),
            dma(others, pieces),
            dma(others, pieces),
            dma(groups),
            dma(groups),
        ],
        compiler_params=pltpu.CompilerParams(collective_id=0, has_side_effects=True),
        name="fused_mixer",
    )(
        q, key_rows[0], value_rows[0], decay_low[0], rate_low[0], decay_up, rate_up,
        decay_base[None], norm_gain[None], out_weight,
    )
    return out[None]


def solution(mesh):
    in_specs = (
        P("dp", "sp", None),
        P("dp", "sp", None),
        P("dp", "sp", None),
        P("dp", "sp", None),
        P("dp", "sp", None),
        P(),
        P(),
        P(),
        P(),
        P(None, "dp"),
    )
    return jax.shard_map(
        functools.partial(per_device, mesh.shape["sp"], mesh.shape["dp"]),
        mesh=mesh, in_specs=in_specs, out_specs=P("dp", "sp", None), check_vma=False,
    )
```

```python
import functools
import math

import jax
import jax.numpy as jnp
from jax import lax
from jax.experimental import pallas as pl
from jax.experimental.pallas import tpu as pltpu
from jax.sharding import PartitionSpec as P

HEAD = 64
PAIR = 2 * HEAD

F32 = jnp.float32
BF16 = jnp.bfloat16


def mm(left, right):
    return lax.dot_general(left, right, (((1,), (0,)), ((), ())), preferred_element_type=F32)


def mm_nt(left, right):
    return lax.dot_general(left, right, (((1,), (1,)), ((), ())), preferred_element_type=F32)


def mm_tn(left, right):
    return lax.dot_general(left, right, (((0,), (0,)), ((), ())), preferred_element_type=F32)


def split(x):
    high = x.astype(BF16)
    return high, (x - high.astype(F32)).astype(BF16)


def mm3(left, right, form=mm):
    return form(left[0], right[0]) + form(left[0], right[1]) + form(left[1], right[0])


def iota(shape, dim):
    return lax.broadcasted_iota(jnp.int32, shape, dim)


def first_half(shape):
    return iota(shape, len(shape) - 1) < HEAD


def stack_pair(x):
    here = lax.rem(iota(x.shape, 1), PAIR) < HEAD
    zero = jnp.zeros_like(x)
    return jnp.concatenate([jnp.where(here, x, zero), jnp.where(here, zero, x)], axis=0)


def head_ones(scale):
    row = iota((2 * PAIR, PAIR), 0)
    col = iota((2 * PAIR, PAIR), 1)
    same = (lax.rem(row, PAIR) // HEAD) == (col // HEAD)
    return jnp.where(same, F32(scale), F32(0.0)).astype(BF16)


def head_sum(x, ones):
    return mm(jnp.concatenate(split(x), axis=1), ones)


def inverse_levels(strict_parts, size):
    row = iota((size, size), 0)
    col = iota((size, size), 1)
    eye = jnp.where(row == col, F32(1.0), F32(0.0))
    found = None
    block = 1
    while block < size:
        pick = (row // (2 * block) == col // (2 * block)) & (row // block != col // block) & (row > col)
        pieces = [jnp.where(pick, high, jnp.zeros_like(high)) for high, _ in strict_parts]
        if found is None:
            found = [eye.astype(BF16) - p for p in pieces]
        else:
            right = [mm(p, x).astype(BF16) for p, x in zip(pieces, found)]
            found = [x - mm(x, y).astype(BF16) for x, y in zip(found, right)]
        block *= 2
    out = []
    for (high, low), x in zip(strict_parts, found):
        product = mm(jnp.concatenate([high, low], axis=1), jnp.concatenate([x, x], axis=0))
        residual = ((eye - x.astype(F32)) - product).astype(BF16)
        out.append((x, mm(x, residual).astype(BF16)))
    return out


def gates(squashed, rate_low, decay_up, rate_up, base):
    decay_pre = (base + mm(squashed, decay_up)).astype(BF16).astype(F32)
    rate_pre = mm(rate_low, rate_up).astype(BF16).astype(F32)
    log_decay = -math.exp(-0.5) / (1.0 + jnp.exp(-decay_pre))
    rate = 1.0 / (1.0 + jnp.exp(-rate_pre))
    return log_decay, rate


def state_pairs(pairs):
    size = pairs[0][0].shape[0]
    middle = size // 2
    row = iota((size, size), 0)
    col = iota((size, size), 1)
    strict = row > col
    upto = jnp.where(row >= col, F32(1.0), F32(0.0)).astype(BF16)
    upto = jnp.concatenate([upto, upto], axis=1)
    ones = head_ones(1.0)
    made = []
    strict_parts = []
    for k, v, log_decay, rate in pairs:
        k = k.astype(F32)
        running = mm(upto, jnp.concatenate(split(log_decay), axis=0))
        centre = running[middle : middle + 1]
        final = running[size - 1 :]
        ahead_before = jnp.exp(running - log_decay - centre)
        behind = jnp.exp(centre - running)
        unit = k * lax.rsqrt(1.0 + head_sum(k * k, ones))
        at_end = jnp.exp(final - centre)
        erase_from = unit * ahead_before
        key_to = k * behind
        erase_to = unit * rate * behind
        left = split(stack_pair(erase_from))
        key_parts, erase_parts = split(key_to), split(erase_to)
        right = [jnp.concatenate(both, axis=0) for both in zip(key_parts, erase_parts)]
        grid = pair_grid(left, right)
        part = lambda i, j: jnp.where(
            strict, grid[i * size : (i + 1) * size, j * size : (j + 1) * size], 0.0
        )
        key_pairs = split(jnp.concatenate([part(0, 0), part(1, 0)], axis=1))
        strict_parts += [split(part(0, 1)), split(part(1, 1))]
        values = stack_pair(v)
        carried = mm(key_pairs[0], values) + mm(key_pairs[1], values)
        sides = jnp.concatenate([erase_from * jnp.exp(centre), carried], axis=1)
        made.append((
            v, sides, key_to * at_end, erase_to * at_end, jnp.exp(final),
            running, key_parts + erase_parts,
        ))
    inverses = inverse_levels(strict_parts, size)
    out = []
    for i, (v, sides, key_end, erase_end, decay_all, running, kept) in enumerate(made):
        xa, xb = inverses[2 * i], inverses[2 * i + 1]
        inv = tuple(jnp.concatenate([a, b], axis=1) for a, b in zip(xa, xb))
        solved = split(mm3(inv, split(stack_pair(sides))))
        key_parts = split(key_end)
        moved = mm3(split(erase_end), solved, mm_tn)
        gained = mm_tn(key_parts[0], v) + mm_tn(key_parts[1], v)
        row2 = iota((PAIR, PAIR), 0)
        col2 = iota((PAIR, PAIR), 1)
        transfer = jnp.where(row2 == col2, jnp.broadcast_to(decay_all, (PAIR, PAIR)), 0.0) - moved[:, :PAIR]
        added = gained - moved[:, PAIR:]
        half = first_half((HEAD, PAIR))
        fold = lambda x: jnp.where(half, x[:HEAD], x[HEAD:])
        halves = tuple(x[:, j : j + PAIR] for j in (0, PAIR) for x in solved)
        out.append((fold(transfer), fold(added), running) + kept + halves)
    return out


def pair_grid(left, right):
    return mm_nt(
        jnp.concatenate(left, axis=1), jnp.concatenate([right[0], right[0]], axis=1)
    ) + mm_nt(left[0], right[1])


def read_pair(q, v, running, kept, start, mean_ones):
    size = q.shape[0]
    within = iota((size, size), 0) >= iota((size, size), 1)
    centre = running[size // 2 : size // 2 + 1]
    read_mid = q.astype(F32) * jnp.exp(running - centre)
    left = split(stack_pair(read_mid))
    right = [jnp.concatenate([kept[i], kept[i + 2]], axis=0) for i in (0, 1)]
    solved = [jnp.concatenate([kept[i + 4], kept[i + 6]], axis=1) for i in (0, 1)]
    grid = pair_grid(left, right)
    part = lambda i, j: jnp.where(
        within, grid[i * size : (i + 1) * size, j * size : (j + 1) * size], 0.0
    )
    read_keys = split(jnp.concatenate([part(0, 0), part(1, 0)], axis=1))
    read_erase = split(jnp.concatenate([part(0, 1), part(1, 1)], axis=1))
    values = stack_pair(v)
    here = mm(read_keys[0], values) + mm(read_keys[1], values)
    taken = mm3(read_erase, [stack_pair(x) for x in solved])
    read_state = read_mid * jnp.exp(centre) - taken[:, :PAIR]
    readout = mm3(split(read_state), split(stack_pair(start))) + here - taken[:, PAIR:]
    centred = readout - head_sum(readout, mean_ones)
    variance = head_sum(centred * centred, mean_ones)
    return centred * lax.rsqrt(variance + 1.0)


def fused_kernel(devices, columns, lanes, pieces, q_ref, k_ref, v_ref, low_ref, rate_ref, dup_ref,
                 rup_ref, base_ref, gain_ref, weight_ref, out_ref, weights, transfer_ref, added_ref,
                 running_ref, kept_ref, mix_ref, start_buf, end_buf, own_sem, near_sem, far_send,
                 far_recv, pass_send, pass_recv, send_sem, recv_sem):
    me = lax.axis_index("sp")
    mine = lax.axis_index("dp")
    partner = mine + 1 - 2 * lax.rem(mine, 2)
    width = q_ref.shape[1]
    groups = width // lanes
    count = lanes // PAIR
    others = columns // 2 - 1
    cols = weight_ref.shape[1]
    piece = weight_ref.shape[0] // pieces
    has_left = me > 0
    has_right = me < devices - 1
    barrier = pltpu.get_barrier_semaphore()

    def greet(where):
        pl.semaphore_signal(barrier, inc=1, device_id=where, device_id_type=pl.DeviceIdType.MESH)

    def ahead_of(j):
        return lax.rem(mine + 2 * (j + 1), columns)

    def behind_of(j):
        return lax.rem(mine + columns - 2 * (j + 1), columns)

    def remote(src, dst, send, recv, where):
        return pltpu.make_async_remote_copy(
            src_ref=src, dst_ref=dst, send_sem=send, recv_sem=recv,
            device_id=where, device_id_type=pl.DeviceIdType.MESH,
        )

    greet({"dp": partner})
    for j in range(others):
        greet({"dp": ahead_of(j)})

    @pl.when(has_left)
    def _():
        greet({"sp": me - 1})

    @pl.when(has_right)
    def _():
        greet({"sp": me + 1})

    own = pltpu.make_async_copy(weight_ref, weights.at[mine], own_sem)
    own.start()
    pl.semaphore_wait(
        barrier, 1 + others + jnp.minimum(me, 1) + jnp.minimum(devices - 1 - me, 1)
    )

    def rows(c):
        return pl.ds(c * piece, piece)

    def far(j, c):
        return remote(
            weight_ref.at[rows(c)], weights.at[mine, rows(c)],
            far_send.at[j, c], far_recv.at[j, c], {"dp": ahead_of(j)},
        )

    def passed(j, c):
        return remote(
            weights.at[behind_of(j), rows(c)], weights.at[behind_of(j), rows(c)],
            pass_send.at[j, c], pass_recv.at[j, c], {"dp": partner},
        )

    near = remote(weight_ref, weights.at[mine], near_sem.at[0], near_sem.at[1], {"dp": partner})
    for j in range(others):
        for c in range(pieces):
            far(j, c).start()
    near.start()

    def forward(c):
        for j in range(others):
            far(j, c).wait_recv()
            passed(j, c).start()

    def lanes_of(g):
        return pl.ds(pl.multiple_of(g * lanes, lanes), lanes)

    def cut(x, i):
        return x[:, i * PAIR : (i + 1) * PAIR]

    def make(g):
        at = lanes_of(g)
        squashed = jnp.tanh(low_ref[...].astype(F32)).astype(BF16)
        log_decay, rate = gates(
            squashed, rate_ref[...], dup_ref[:, at], rup_ref[:, at], base_ref[:, at]
        )
        k, v = k_ref[:, at], v_ref[:, at]
        pairs = [tuple(cut(x, i) for x in (k, v, log_decay, rate)) for i in range(count)]
        parts = [jnp.concatenate(part, axis=1) for part in zip(*state_pairs(pairs))]
        transfer_ref[:, at], added_ref[:, at], running_ref[:, at] = parts[:3]
        for i, part in enumerate(parts[3:]):
            kept_ref[i, :, at] = part

    def copy(g):
        return remote(
            end_buf.at[g], start_buf.at[g], send_sem.at[g], recv_sem.at[g],
            {"sp": lax.rem(me + 1, devices)},
        )

    def advance(g):
        @pl.when(has_left)
        def _():
            copy(g).wait_recv()

        at = lanes_of(g)
        transfer, added, start = transfer_ref[:, at], added_ref[:, at], start_buf[g]
        ends = [
            mm3(split(cut(transfer, i)), split(stack_pair(cut(start, i)))) for i in range(count)
        ]
        end_buf[g] = jnp.concatenate(ends, axis=1) + added

        @pl.when(has_right)
        def _():
            copy(g).start()

    mean_ones = head_ones(1.0 / HEAD)

    def read(g):
        at = lanes_of(g)
        q, v, running, gain, start = (
            q_ref[:, at], v_ref[:, at], running_ref[:, at], gain_ref[:, at], start_buf[g]
        )
        kept = [kept_ref[j, :, at] for j in range(kept_ref.shape[0])]
        normed = [
            read_pair(
                cut(q, i), cut(v, i), cut(running, i), [cut(x, i) for x in kept],
                cut(start, i), mean_ones,
            )
            for i in range(count)
        ]
        mix_ref[:, at] = (jnp.concatenate(normed, axis=1) * gain).astype(BF16)

    @pl.when(jnp.logical_not(has_left))
    def _():
        start_buf[...] = jnp.zeros_like(start_buf)

    slots = max(groups, devices) + groups
    early = min(pieces, (slots - 1) // 4)

    def slot(s, carry):
        @pl.when(s < groups)
        def _():
            make(s)

        @pl.when((s >= me) & (s < me + groups))
        def _():
            advance(s - me)

        first = jnp.maximum(groups, me + 1)

        @pl.when((s >= first) & (s < first + groups))
        def _():
            read(s - first)

        c = s // 4 - 1

        @pl.when((lax.rem(s, 4) == 0) & (c >= 0) & (c < early))
        def _():
            forward(c)

        return carry

    lax.fori_loop(0, slots, slot, 0)
    for c in range(early, pieces):
        forward(c)

    def project(d):
        at = pl.ds(pl.multiple_of(d * cols, cols), cols)
        out_ref[:, at] = mm(mix_ref[...], weights[d]).astype(BF16)

    own.wait()
    project(mine)
    near.wait_recv()
    project(partner)
    for j in range(others):
        project(behind_of(j))
    for j in range(others):
        for c in range(pieces):
            passed(j, c).wait_recv()
        project(lax.rem(partner + columns - 2 * (j + 1), columns))

    near.wait_send()
    for j in range(others):
        for c in range(pieces):
            far(j, c).wait_send()
            passed(j, c).wait_send()

    @pl.when(has_right)
    def _():
        for g in range(groups):
            copy(g).wait_send()


def per_device(devices, columns, query_rows, key_rows, value_rows, decay_low, rate_low, decay_up,
               rate_up, decay_base, norm_gain, out_weight):
    q = query_rows[0]
    size, width = q.shape
    depth, cols = out_weight.shape
    lanes = PAIR * math.gcd(width // PAIR, 2)
    groups = width // lanes
    pieces = 4
    others = columns // 2 - 1
    vmem = pl.BlockSpec(memory_space=pltpu.VMEM)
    dma = lambda *dims: pltpu.SemaphoreType.DMA(dims)
    out = pl.pallas_call(
        functools.partial(fused_kernel, devices, columns, lanes, pieces),
        in_specs=[vmem] * 9 + [pl.BlockSpec(memory_space=pl.ANY)],
        out_specs=vmem,
        out_shape=jax.ShapeDtypeStruct((size, columns * cols), BF16),
        scratch_shapes=[
            pltpu.VMEM((columns, depth, cols), BF16),
            pltpu.VMEM((HEAD, width), F32),
            pltpu.VMEM((HEAD, width), F32),
            pltpu.VMEM((size, width), F32),
            pltpu.VMEM((8, size, width), BF16),
            pltpu.VMEM((size, width), BF16),
            pltpu.VMEM((groups, HEAD, lanes), F32),
            pltpu.VMEM((groups, HEAD, lanes), F32),
            pltpu.SemaphoreType.DMA,
            dma(2),
            dma(others, pieces),
            dma(others, pieces),
            dma(others, pieces),
            dma(others, pieces),
            dma(groups),
            dma(groups),
        ],
        compiler_params=pltpu.CompilerParams(collective_id=0, has_side_effects=True),
        name="fused_mixer",
    )(
        q, key_rows[0], value_rows[0], decay_low[0], rate_low[0], decay_up, rate_up,
        decay_base[None], norm_gain[None], out_weight,
    )
    return out[None]


def solution(mesh):
    in_specs = (
        P("dp", "sp", None),
        P("dp", "sp", None),
        P("dp", "sp", None),
        P("dp", "sp", None),
        P("dp", "sp", None),
        P(),
        P(),
        P(),
        P(),
        P(None, "dp"),
    )
    return jax.shard_map(
        functools.partial(per_device, mesh.shape["sp"], mesh.shape["dp"]),
        mesh=mesh, in_specs=in_specs, out_specs=P("dp", "sp", None), check_vma=False,
    )
```
